32 devices in a mesh: fs: 8 (over z, x), tp: 4 (over y, core).
Axes of the slice: x: 2, y: 2, z: 4, core: 2. Of those that a mesh axis runs over, the one named last changes fastest.
Arguments:
- tokens: bfloat16 [4096, 2048], P('fs', 'tp'), may hold values from -16 to 16
- pre_mix_gain: bfloat16 [2048], P('tp'), may hold values from 0.099609375 to 1.8984375
- w_gate_in: bfloat16 [2048, 2048], P('fs', 'tp'), may hold values from -0.125 to 0.125
- w_input: bfloat16 [2048, 2048], P('fs', 'tp'), may hold values from -0.125 to 0.125
- mix_kernel: bfloat16 [4, 2048], P(None, 'tp'), may hold values from -3 to 3
- w_recur: bfloat16 [8, 256, 256], P('tp'), may hold values from -0.375 to 0.375
- w_inject: bfloat16 [8, 256, 256], P('tp'), may hold values from -0.375 to 0.375
- decay_param: float32 [2048], P('tp'), may hold values from 3 to 13
- w_mix_out: bfloat16 [2048, 2048], P('tp', 'fs'), may hold values from -0.125 to 0.125
- post_mix_gain: bfloat16 [2048], P('tp'), may hold values from 0.099609375 to 1.8984375
- pre_ffn_gain: bfloat16 [2048], P('tp'), may hold values from 0.099609375 to 1.8984375
- w_up_gate: bfloat16 [2048, 5632], P('fs', 'tp'), may hold values from -0.125 to 0.125
- w_up_value: bfloat16 [2048, 5632], P('fs', 'tp'), may hold values from -0.125 to 0.125
- gate_kernel: bfloat16 [3, 5632], P(None, 'tp'), may hold values from -3 to 3
- value_kernel: bfloat16 [3, 5632], P(None, 'tp'), may hold values from -3 to 3
- w_down: bfloat16 [5632, 2048], P('tp', 'fs'), may hold values from -0.078125 to 0.078125
- post_ffn_gain: bfloat16 [2048], P('tp'), may hold values from 0.099609375 to 1.8984375
Outputs:
- layer_out: bfloat16 [4096, 2048], P('fs', 'tp')
The draws below stay inside these ranges and needn't reach their ends.
All inputs are finite; a program needn't handle non-finite values.
Results may differ from the reference program's by a relative error of at most 0.015.
Values may be sent and summed in bfloat16 or wider, within the bound.
A program may use at most 64 MiB of HBM per device.

```python
import math
import jax
import jax.numpy as jnp
from jax import lax

D = 2048
HEADS = 8
HEAD_SIZE = 256
W = 2048
FF = 5632
MIX_TAPS = 4
FFN_TAPS = 3
LEN = 512
TOKENS = 4096
N_FS = 8
N_TP = 4


gate_power = 8.0


def draw_tokens(key, part):
    keys = jax.random.split(key, 6)
    levels = 0.5 * 4.0 ** (jnp.arange(8, dtype=jnp.float32) / 7.0)
    order = jax.random.permutation(keys[0], 8)
    channel_scale = levels[order][jnp.arange(D) // (D // 8)]
    noise = jax.random.normal(keys[1], (TOKENS, D), jnp.float32)
    direction = jax.random.normal(keys[2], (D,), jnp.float32)
    shift = jax.random.normal(keys[3], (TOKENS // 16, 1), jnp.float32) * 1.5
    shift = jnp.repeat(shift, 16, axis=0)
    values = noise * channel_scale[None, :] + shift * direction[None, :]
    return jnp.clip(values, -16.0, 16.0).astype(jnp.bfloat16)


def draw_decay_param(key, part):
    keys = jax.random.split(key, 3)
    slow = jnp.exp(jax.random.uniform(keys[0], (W,), jnp.float32, math.log(0.1), math.log(2.0))) / (gate_power * LEN)
    fast = jnp.exp(jax.random.uniform(keys[1], (W,), jnp.float32, math.log(0.01), math.log(0.04)))
    picks = jax.random.randint(keys[2], (W,), 0, 2) == 1
    rate = jnp.where(picks, fast, slow)
    return (-jnp.log(jnp.expm1(rate))).astype(jnp.float32)


def steps_of(stream_key, shape, cuts, low, largest):
    loudness, own = 1.0, jax.random.fold_in(stream_key, 6)
    for axis_at, parts in cuts:
        draws = jnp.exp(jax.random.uniform(jax.random.fold_in(own, axis_at), (parts,), jnp.float32, low / len(cuts), largest / len(cuts)))
        loudness = loudness * jnp.repeat(draws, shape[axis_at] // parts).reshape([-1 if axis == axis_at else 1 for axis in range(len(shape))])
    return loudness


def centred(rng, dims, spread, reach, cuts=(), held_as=jnp.bfloat16):
    values = jax.random.normal(rng, dims, jnp.float32) * spread
    if len(cuts) > 0:
        values = steps_of(rng, dims, cuts, -0.22, 0.18) * values
    return jnp.clip(values, min=-reach, max=reach).astype(held_as)


def setup_inputs(seed: int = 0) -> dict:
    arg_keys = jax.random.split(jax.random.key(seed), 18)
    return {
        "tokens": draw_tokens(jax.random.fold_in(arg_keys[17], 71), 0),
        "pre_mix_gain": jnp.clip(1.0 + 0.18 * jax.random.normal(arg_keys[1], (D,), jnp.float32), 0.099609375, 1.8984375).astype(jnp.bfloat16),
        "w_gate_in": centred(arg_keys[2], (D, W), D ** -0.5, 0.125, ((0, 8), (1, 4))),
        "w_input": centred(arg_keys[3], (D, W), D ** -0.5, 0.125, ((0, 8), (1, 4))),
        "mix_kernel": centred(arg_keys[4], (MIX_TAPS, W), 0.5, 3.0, ((1, 4),)),
        "w_recur": centred(arg_keys[5], (HEADS, HEAD_SIZE, HEAD_SIZE), HEAD_SIZE ** -0.5, 0.375, ((0, 4),)),
        "w_inject": centred(arg_keys[6], (HEADS, HEAD_SIZE, HEAD_SIZE), HEAD_SIZE ** -0.5, 0.375, ((0, 4),)),
        "decay_param": draw_decay_param(jax.random.fold_in(arg_keys[17], 71), 0),
        "w_mix_out": centred(arg_keys[8], (W, D), W ** -0.5, 0.125, ((0, 4), (1, 8))),
        "post_mix_gain": jnp.clip(1.0 + 0.18 * jax.random.normal(arg_keys[9], (D,), jnp.float32), 0.099609375, 1.8984375).astype(jnp.bfloat16),
        "pre_ffn_gain": jnp.clip(1.0 + 0.18 * jax.random.normal(arg_keys[10], (D,), jnp.float32), 0.099609375, 1.8984375).astype(jnp.bfloat16),
        "w_up_gate": centred(arg_keys[11], (D, FF), D ** -0.5, 0.125, ((0, 8), (1, 4))),
        "w_up_value": centred(arg_keys[12], (D, FF), D ** -0.5, 0.125, ((0, 8), (1, 4))),
        "gate_kernel": centred(arg_keys[13], (FFN_TAPS, FF), 0.577, 3.0, ((1, 4),)),
        "value_kernel": centred(arg_keys[14], (FFN_TAPS, FF), 0.577, 3.0, ((1, 4),)),
        "w_down": centred(arg_keys[15], (FF, D), FF ** -0.5, 0.078125, ((0, 4), (1, 8))),
        "post_ffn_gain": jnp.clip(1.0 + 0.18 * jax.random.normal(arg_keys[16], (D,), jnp.float32), 0.099609375, 1.8984375).astype(jnp.bfloat16),
    }


norm_eps = 1e-06
gate_power = 8.0

def row_normed(values, row_gain):
    widened = values.astype(jnp.float32)
    squares = lax.optimization_barrier(jnp.sum(widened * widened, axis=1))
    factor = lax.rsqrt(squares / D + norm_eps)
    return widened * factor[:, None] * row_gain.astype(jnp.float32)[None, :]

def causal_conv(values, kernel):
    length = values.shape[0]
    widths = kernel.shape[0]
    padded = jnp.pad(values.astype(jnp.float32), ((widths - 1, 0), (0, 0)))
    weights = kernel.astype(jnp.float32)
    result = padded[0:length] * weights[0]
    for offset in range(1, widths):
        result = result + padded[offset:offset + length] * weights[offset]
    return result

def linear_combine(earlier, latter):
    return (earlier[0] * latter[0], latter[0] * earlier[1] + latter[1])

def split_sum(activ, weight):
    length = activ.shape[0]
    blocks = activ.reshape(length, N_TP, -1).transpose(1, 0, 2).astype(jnp.float32)
    wblocks = weight.reshape(N_TP, -1, weight.shape[1]).astype(jnp.float32)
    partial_value = jnp.einsum('ktw,kwd->ktd', blocks, wblocks)
    partial_value = partial_value.astype(jnp.bfloat16).astype(jnp.float32)
    return lax.optimization_barrier(jnp.sum(partial_value, axis=0))

def reference(tokens, pre_mix_gain, w_gate_in, w_input, mix_kernel, w_recur, w_inject, decay_param, w_mix_out, post_mix_gain, pre_ffn_gain, w_up_gate, w_up_value, gate_kernel, value_kernel, w_down, post_ffn_gain):
    sequences = tokens.reshape(N_FS, LEN, D)

    def one_sequence(rows):
        normed_in = row_normed(rows, pre_mix_gain).astype(jnp.bfloat16)
        gate_rows = jnp.dot(normed_in, w_gate_in, preferred_element_type=jnp.float32).astype(jnp.bfloat16)
        input_rows = jnp.dot(normed_in, w_input, preferred_element_type=jnp.float32).astype(jnp.bfloat16)
        smoothed = causal_conv(input_rows, mix_kernel).astype(jnp.bfloat16)
        by_head = smoothed.reshape(LEN, HEADS, HEAD_SIZE).astype(jnp.float32)
        recur_gate = jax.nn.sigmoid(jnp.einsum('thi,hij->thj', by_head, w_recur.astype(jnp.float32))).reshape(LEN, W)
        inject_gate = jax.nn.sigmoid(jnp.einsum('thi,hij->thj', by_head, w_inject.astype(jnp.float32))).reshape(LEN, W)
        log_retain = -gate_power * recur_gate * jax.nn.softplus(-decay_param.astype(jnp.float32))[None, :]
        retain = jnp.exp(log_retain)
        driven = jnp.sqrt(-jnp.expm1(2.0 * log_retain)) * inject_gate * smoothed.astype(jnp.float32)
        _, states = lax.associative_scan(linear_combine, (retain, driven), axis=0)
        hidden = (jax.nn.gelu(gate_rows.astype(jnp.float32), approximate=True) * states).astype(jnp.bfloat16)
        mixer_sum = split_sum(hidden, w_mix_out)
        middle = (rows.astype(jnp.float32) + row_normed(mixer_sum, post_mix_gain)).astype(jnp.bfloat16)
        normed_mid = row_normed(middle, pre_ffn_gain).astype(jnp.bfloat16)
        up_gate = jnp.dot(normed_mid, w_up_gate, preferred_element_type=jnp.float32).astype(jnp.bfloat16)
        up_value = jnp.dot(normed_mid, w_up_value, preferred_element_type=jnp.float32).astype(jnp.bfloat16)
        conv_g = causal_conv(up_gate, gate_kernel)
        conv_v = causal_conv(up_value, value_kernel)
        activated = (jax.nn.gelu(conv_g, approximate=True) * conv_v).astype(jnp.bfloat16)
        ffn_sum = split_sum(activated, w_down)
        return (middle.astype(jnp.float32) + row_normed(ffn_sum, post_ffn_gain)).astype(jnp.bfloat16)
    return lax.map(one_sequence, sequences).reshape(N_FS * LEN, D)
```

```python
import functools

import jax
import jax.numpy as jnp
from jax import lax
from jax.experimental import pallas as pl
from jax.experimental.pallas import tpu as pltpu
from jax.sharding import PartitionSpec as P


norm_eps = 1e-06
gate_power = 8.0
f32 = jnp.float32
bf16 = jnp.bfloat16


def normed_full(values, row_gain):
    widened = values.astype(f32)
    squares = jnp.sum(widened * widened, axis=1)
    factor = lax.rsqrt(squares / values.shape[1] + norm_eps)
    return widened * factor[:, None] * row_gain.astype(f32)[None, :]


def ring_order(n):
    return list(range(0, n, 2)) + list(range(1, n, 2))[::-1]


def bit_pairs(n, bit):
    return [(i, i ^ bit) for i in range(n)]


def swapped(value, n, bit):
    return lax.ppermute(value, "tp", bit_pairs(n, bit))


def paired(mine, theirs, index, bit, axis):
    low = (index & bit) == 0
    return jnp.stack([jnp.where(low, mine, theirs), jnp.where(low, theirs, mine)], axis=axis)


def bits_up(n):
    bits, bit = [], 1
    while bit < n:
        bits.append(bit)
        bit *= 2
    return bits


def gathered_columns(block, n, index):
    rows, width = block.shape
    held = block[None]
    lead = 0
    for bit in reversed(bits_up(n)):
        held = paired(held, swapped(held, n, bit), index, bit, 1)
        held = held.reshape((-1,) + block.shape)
    return held.transpose(1, 0, 2).reshape(rows, n * width)


def gathered_rows(block, n, index):
    held = block
    for bit in reversed(bits_up(n)):
        held = paired(held, swapped(held, n, bit), index, bit, 0).reshape(-1, block.shape[1])
    return held


def scattered_rows(partial_value, n, index):
    held = partial_value
    for bit in bits_up(n):
        halves = held.astype(bf16).reshape(2, -1, held.shape[1])
        side = (index & bit) // bit
        keep = lax.dynamic_index_in_dim(halves, side, 0, keepdims=False)
        send = lax.dynamic_index_in_dim(halves, 1 - side, 0, keepdims=False)
        held = keep.astype(f32) + swapped(send, n, bit).astype(f32)
    return held


def scattered_columns(partial_value, n, index):
    rows = partial_value.shape[0]
    held = partial_value.reshape(rows, n, -1).transpose(1, 0, 2)
    for bit in bits_up(n):
        halves = held.astype(bf16).reshape((-1, 2) + held.shape[1:])
        side = (index & bit) // bit
        keep = lax.dynamic_index_in_dim(halves, side, 1, keepdims=False)
        send = lax.dynamic_index_in_dim(halves, 1 - side, 1, keepdims=False)
        held = keep.astype(f32) + swapped(send, n, bit).astype(f32)
    return held[0]


class Ring:
    def __init__(self, n):
        self.n = n
        self.order = ring_order(n)
        places = [0] * n
        for place, member in enumerate(self.order):
            places[member] = place
        self.place = jnp.asarray(places, jnp.int32)[lax.axis_index("fs")]
        self.members = jnp.asarray(self.order, jnp.int32)
        self.right = [(self.order[i], self.order[(i + 1) % n]) for i in range(n)]
        self.left = [(b, a) for a, b in self.right]

    def owner(self, shift):
        return self.members[(self.place + shift + self.n) % self.n]

    def gather(self, shards, after=None):
        if after is not None:
            shards = lax.optimization_barrier(tuple(shards) + (after,))[:-1]
        found = [[(0, shard)] for shard in shards]
        ahead = list(shards)
        back = list(shards)
        far = self.n // 2
        marks = []
        for step in range(1, far + 1):
            for at in range(len(shards)):
                both = 2 * step < self.n
                if both or at % 2 == 0:
                    ahead[at] = lax.ppermute(ahead[at], "fs", self.right)
                    found[at].append((-step, ahead[at]))
                if both or at % 2 == 1:
                    back[at] = lax.ppermute(back[at], "fs", self.left)
                    found[at].append((step, back[at]))
            marks.append(found[-1][-1][1])
        return found, marks


def summed_chunks(ring, inputs, found):
    depth = found[0][1].shape[0]
    total = None
    for shift, shard in found:
        part = lax.dynamic_slice_in_dim(inputs, ring.owner(shift) * depth, depth, axis=1)
        term = jnp.dot(part, shard, preferred_element_type=f32)
        total = term if total is None else total + term
    return total.astype(bf16)


def placed_chunks(ring, inputs, found):
    width = found[0][1].shape[1]
    result = jnp.zeros((inputs.shape[0], ring.n * width), bf16)
    for shift, shard in found:
        term = jnp.dot(inputs, shard, preferred_element_type=f32).astype(bf16)
        result = lax.dynamic_update_slice_in_dim(result, term, ring.owner(shift) * width, axis=1)
    return result


def shifted(values, by):
    rows = lax.broadcasted_iota(jnp.int32, values.shape, 0)
    return jnp.where(rows >= by, pltpu.roll(values, by, 0), 0.0)


def minus_expm1(y):
    series = 1.0 / 10.0
    total = 1.0 + y * series
    for k in range(9, 1, -1):
        total = 1.0 + y * total * (1.0 / k)
    return jnp.where(y > -0.9, -y * total, 1.0 - jnp.exp(y))


def gelu(x):
    return 0.5 * x * (1.0 + jnp.tanh(0.7978845608028654 * (x + 0.044715 * (x * x * x))))


def mixer_kernel(gate_ref, input_ref, taps_ref, recur_ref, inject_ref, soft_ref, out_ref, a_ref, b_ref):
    length = gate_ref.shape[0]
    taps = taps_ref.shape[0]
    weights = taps_ref[...].astype(f32)
    values = input_ref[...].astype(f32)
    total = values * weights[taps - 1 : taps]
    for back in range(1, taps):
        total = total + shifted(values, back) * weights[taps - 1 - back : taps - back]
    smoothed = total.astype(bf16)
    recur = jax.nn.sigmoid(jnp.dot(smoothed, recur_ref[0], preferred_element_type=f32))
    log_retain = -gate_power * recur * soft_ref[...]
    inject = jax.nn.sigmoid(jnp.dot(smoothed, inject_ref[0], preferred_element_type=f32))
    a = jnp.exp(log_retain)
    b = jnp.sqrt(minus_expm1(2.0 * log_retain)) * inject * smoothed.astype(f32)
    inner = lax.broadcasted_iota(jnp.int32, a.shape, 0) % 8
    for by in (1, 2, 4):
        inside = inner >= by
        b = b + a * jnp.where(inside, pltpu.roll(b, by, 0), 0.0)
        a = a * jnp.where(inside, pltpu.roll(a, by, 0), 1.0)
    a_ref[...] = a
    b_ref[...] = b

    def group(at, carry):
        rows = pl.ds(pl.multiple_of(at * 8, 8), 8)
        states = a_ref[rows, :] * carry + b_ref[rows, :]
        b_ref[rows, :] = states
        return states[7:8, :]

    lax.fori_loop(0, length // 8, group, jnp.zeros((1, a.shape[1]), f32), unroll=4)
    out_ref[...] = (gelu(gate_ref[...].astype(f32)) * b_ref[...]).astype(bf16)


def mixed(gate_rows, input_rows, mix_kernel, w_recur, w_inject, soft):
    length, width = gate_rows.shape
    heads, size, _ = w_recur.shape
    across = pl.BlockSpec((length, size), lambda h: (0, h))
    block = pl.BlockSpec((1, size, size), lambda h: (h, 0, 0))
    return pl.pallas_call(
        mixer_kernel,
        grid=(heads,),
        out_shape=jax.ShapeDtypeStruct((length, width), bf16),
        in_specs=[
            across,
            across,
            pl.BlockSpec((mix_kernel.shape[0], size), lambda h: (0, h)),
            block,
            block,
            pl.BlockSpec((1, size), lambda h: (0, h)),
        ],
        out_specs=across,
        scratch_shapes=[pltpu.VMEM((length, size), f32), pltpu.VMEM((length, size), f32)],
        cost_estimate=pl.CostEstimate(
            flops=20_000_000 * heads, bytes_accessed=4 * length * width * 2, transcendentals=0
        ),
    )(gate_rows, input_rows, mix_kernel, w_recur, w_inject, soft)


def causal_conv(values, kernel):
    length = values.shape[0]
    widths = kernel.shape[0]
    padded = jnp.pad(values.astype(f32), ((widths - 1, 0), (0, 0)))
    weights = kernel.astype(f32)
    result = padded[0:length] * weights[0]
    for offset in range(1, widths):
        result = result + padded[offset : offset + length] * weights[offset]
    return result


def shards(
    n_fs,
    n_tp,
    tokens,
    pre_mix_gain,
    w_gate_in,
    w_input,
    mix_kernel,
    w_recur,
    w_inject,
    decay_param,
    w_mix_out,
    post_mix_gain,
    pre_ffn_gain,
    w_up_gate,
    w_up_value,
    gate_kernel,
    value_kernel,
    w_down,
    post_ffn_gain,
):
    index = lax.axis_index("tp")
    ring = Ring(n_fs)
    length, width = tokens.shape

    gains = jnp.stack([pre_mix_gain, post_mix_gain, pre_ffn_gain])
    gains = jnp.pad(gains, ((0, 13), (0, 0)))
    rows_all = gathered_columns(jnp.concatenate([tokens, gains], axis=0), n_tp, index)
    tokens_all = rows_all[:length]
    pre_mix_all, post_mix_all, pre_ffn_all = rows_all[length], rows_all[length + 1], rows_all[length + 2]

    in_found, in_marks = ring.gather([w_input, w_gate_in])
    out_found, out_marks = ring.gather([w_mix_out], after=in_marks[-1])
    up_found, up_marks = ring.gather([w_up_gate, w_up_value], after=out_marks[-2])
    down_found, _ = ring.gather([w_down], after=up_marks[-1])

    normed_in = normed_full(tokens_all, pre_mix_all).astype(bf16)
    input_rows = summed_chunks(ring, normed_in, in_found[0])
    gate_rows = summed_chunks(ring, normed_in, in_found[1])
    soft = jax.nn.softplus(-decay_param)[None, :]
    hidden = mixed(gate_rows, input_rows, mix_kernel, w_recur, w_inject, soft)
    mixer_rows = scattered_rows(placed_chunks(ring, hidden, out_found[0]), n_tp, index)

    place = jnp.int32(0)
    rows = length
    for bit in bits_up(n_tp):
        rows //= 2
        place = place + ((index & bit) // bit) * rows
    my_tokens = lax.dynamic_slice_in_dim(tokens_all, place, rows, axis=0)
    my_middle = (my_tokens.astype(f32) + normed_full(mixer_rows, post_mix_all)).astype(bf16)
    middle = gathered_rows(my_middle, n_tp, index)
    normed_mid = normed_full(middle, pre_ffn_all).astype(bf16)

    up_gate = summed_chunks(ring, normed_mid, up_found[0])
    up_value = summed_chunks(ring, normed_mid, up_found[1])
    activated = (
        jax.nn.gelu(causal_conv(up_gate, gate_kernel), approximate=True)
        * causal_conv(up_value, value_kernel)
    ).astype(bf16)
    activated = lax.optimization_barrier(activated)
    ffn_sum = scattered_columns(placed_chunks(ring, activated, down_found[0]), n_tp, index)
    squares = lax.psum(jnp.sum(ffn_sum * ffn_sum, axis=1), "tp")
    factor = lax.rsqrt(squares / (width * n_tp) + norm_eps)
    mine = lax.dynamic_slice_in_dim(middle, index * width, width, axis=1)
    return (
        mine.astype(f32) + ffn_sum * factor[:, None] * post_ffn_gain.astype(f32)[None, :]
    ).astype(bf16)


def solution(mesh):
    return jax.shard_map(
        functools.partial(shards, mesh.shape["fs"], mesh.shape["tp"]),
        mesh=mesh,
        in_specs=(
            P("fs", "tp"),
            P("tp"),
            P("fs", "tp"),
            P("fs", "tp"),
            P(None, "tp"),
            P("tp", None, None),
            P("tp", None, None),
            P("tp"),
            P("tp", "fs"),
            P("tp"),
            P("tp"),
            P("fs", "tp"),
            P("fs", "tp"),
            P(None, "tp"),
            P(None, "tp"),
            P("tp", "fs"),
            P("tp"),
        ),
        out_specs=P("fs", "tp"),
        check_vma=False,
    )
```

```python
import jax
import jax.numpy as jnp
from jax import lax
from jax.experimental import pallas as pl
from jax.experimental.pallas import tpu as pltpu
from jax.sharding import PartitionSpec as P


norm_eps = 1e-06
gate_power = 8.0
f32 = jnp.float32
bf16 = jnp.bfloat16


def normed_full(values, row_gain):
    widened = values.astype(f32)
    squares = jnp.sum(widened * widened, axis=1)
    factor = lax.rsqrt(squares / values.shape[1] + norm_eps)
    return widened * factor[:, None] * row_gain.astype(f32)[None, :]


def ring_order(n):
    return list(range(0, n, 2)) + list(range(1, n, 2))[::-1]


def bit_pairs(n, bit):
    return [(i, i ^ bit) for i in range(n)]


def swapped(value, n, bit):
    return lax.ppermute(value, "tp", bit_pairs(n, bit))


def paired(mine, theirs, index, bit, axis):
    low = (index & bit) == 0
    return jnp.stack([jnp.where(low, mine, theirs), jnp.where(low, theirs, mine)], axis=axis)


def bits_up(n):
    bits, bit = [], 1
    while bit < n:
        bits.append(bit)
        bit *= 2
    return bits


def gathered_columns(block, n, index):
    rows, width = block.shape
    held = block[None]
    for bit in reversed(bits_up(n)):
        held = paired(held, swapped(held, n, bit), index, bit, 1)
        held = held.reshape((-1,) + block.shape)
    return held.transpose(1, 0, 2).reshape(rows, n * width)


def gathered_rows(block, n, index):
    held = block
    for bit in reversed(bits_up(n)):
        held = paired(held, swapped(held, n, bit), index, bit, 0).reshape(-1, block.shape[1])
    return held


def scattered_rows(chunks, n, index):
    held = chunks
    for bit in bits_up(n):
        halves = held.astype(bf16).reshape(held.shape[0], 2, -1, held.shape[2])
        side = (index & bit) // bit
        keep = lax.dynamic_index_in_dim(halves, side, 1, keepdims=False)
        send = lax.dynamic_index_in_dim(halves, 1 - side, 1, keepdims=False)
        held = keep.astype(f32) + swapped(send, n, bit).astype(f32)
    return held.transpose(1, 0, 2).reshape(held.shape[1], -1)


def scattered_columns(chunks, n, index):
    held = chunks.reshape((n, -1) + chunks.shape[1:])
    for bit in bits_up(n):
        halves = held.astype(bf16).reshape((-1, 2) + held.shape[1:])
        side = (index & bit) // bit
        keep = lax.dynamic_index_in_dim(halves, side, 1, keepdims=False)
        send = lax.dynamic_index_in_dim(halves, 1 - side, 1, keepdims=False)
        held = keep.astype(f32) + swapped(send, n, bit).astype(f32)
    return held[0].transpose(1, 0, 2).reshape(chunks.shape[1], -1)


class Ring:
    def __init__(self, n):
        self.n = n
        self.order = ring_order(n)
        places = [0] * n
        for place, member in enumerate(self.order):
            places[member] = place
        self.place = jnp.asarray(places, jnp.int32)[lax.axis_index("fs")]
        self.members = jnp.asarray(self.order, jnp.int32)
        self.right = [(self.order[i], self.order[(i + 1) % n]) for i in range(n)]
        self.left = [(b, a) for a, b in self.right]

    def owner(self, shift):
        return self.members[(self.place + shift + self.n) % self.n]

    def start(self, name, shards, after=None):
        if after is not None:
            shards = lax.optimization_barrier(tuple(shards) + tuple(after))[: len(shards)]
        shards = list(shards)
        return {"name": name, "step": 0, "found": [[(0, x)] for x in shards], "ahead": shards, "back": list(shards)}

    def advance(self, state, rounds=1):
        ahead, back, found = state["ahead"], state["back"], state["found"]
        for _ in range(rounds):
            state["step"] += 1
            step = state["step"]
            for at in range(len(ahead)):
                if 2 * step < self.n:
                    ahead[at] = lax.ppermute(ahead[at], "fs", self.right)
                    back[at] = lax.ppermute(back[at], "fs", self.left)
                    found[at] += [(-step, ahead[at]), (step, back[at])]
                elif len(ahead) == 1:
                    half = ahead[at].shape[0] // 2
                    top = lax.ppermute(ahead[at][:half], "fs", self.right)
                    bottom = lax.ppermute(back[at][half:], "fs", self.left)
                    found[at].append((step, jnp.concatenate([top, bottom], axis=0)))
                elif at % 2 == 0:
                    ahead[at] = lax.ppermute(ahead[at], "fs", self.right)
                    found[at].append((-step, ahead[at]))
                else:
                    back[at] = lax.ppermute(back[at], "fs", self.left)
                    found[at].append((step, back[at]))
        return state

    def marks(self, state):
        return tuple(state["ahead"]) + tuple(state["back"])

    def tie(self, state, value):
        count = len(state["ahead"])
        tied = lax.optimization_barrier((value,) + self.marks(state))
        state["ahead"], state["back"] = list(tied[1 : 1 + count]), list(tied[1 + count :])
        return tied[0]


def summed_chunks(ring, inputs, found):
    depth = found[0][1].shape[0]
    total = None
    for shift, shard in found:
        part = lax.dynamic_slice_in_dim(inputs, ring.owner(shift) * depth, depth, axis=1)
        term = jnp.dot(part, shard, preferred_element_type=f32)
        total = term if total is None else total + term
    return total.astype(bf16)


def placed_chunks(ring, inputs, found):
    width = found[0][1].shape[1]
    result = jnp.zeros((ring.n, inputs.shape[0], width), bf16)
    for shift, shard in found:
        term = jnp.dot(inputs, shard, preferred_element_type=f32).astype(bf16)
        result = lax.dynamic_update_slice_in_dim(result, term[None], ring.owner(shift), axis=0)
    return result


def shifted(values, by):
    rows = lax.broadcasted_iota(jnp.int32, values.shape, 0)
    return jnp.where(rows >= by, pltpu.roll(values, by, 0), 0.0)


def minus_expm1(y):
    series = 1.0 / 10.0
    total = 1.0 + y * series
    for k in range(9, 1, -1):
        total = 1.0 + y * total * (1.0 / k)
    return jnp.where(y > -0.9, -y * total, 1.0 - jnp.exp(y))


def gelu(x):
    return 0.5 * x * (1.0 + jnp.tanh(0.7978845608028654 * (x + 0.044715 * (x * x * x))))


def mixer_kernel(gate_ref, input_ref, taps_ref, recur_ref, inject_ref, soft_ref, out_ref, a_ref, b_ref):
    length = gate_ref.shape[0]
    taps = taps_ref.shape[0]
    weights = taps_ref[...].astype(f32)
    values = input_ref[...].astype(f32)
    total = values * weights[taps - 1 : taps]
    for back in range(1, taps):
        total = total + shifted(values, back) * weights[taps - 1 - back : taps - back]
    smoothed = total.astype(bf16)
    recur = jax.nn.sigmoid(jnp.dot(smoothed, recur_ref[0], preferred_element_type=f32))
    log_retain = -gate_power * recur * soft_ref[...]
    inject = jax.nn.sigmoid(jnp.dot(smoothed, inject_ref[0], preferred_element_type=f32))
    a = jnp.exp(log_retain)
    b = jnp.sqrt(minus_expm1(2.0 * log_retain)) * inject * smoothed.astype(f32)
    inner = lax.broadcasted_iota(jnp.int32, a.shape, 0) % 8
    for by in (1, 2, 4):
        inside = inner >= by
        b = b + a * jnp.where(inside, pltpu.roll(b, by, 0), 0.0)
        a = a * jnp.where(inside, pltpu.roll(a, by, 0), 1.0)
    a_ref[...] = a
    b_ref[...] = b

    def group(at, carry):
        rows = pl.ds(pl.multiple_of(at * 8, 8), 8)
        states = a_ref[rows, :] * carry + b_ref[rows, :]
        b_ref[rows, :] = states
        return states[7:8, :]

    lax.fori_loop(0, length // 8, group, jnp.zeros((1, a.shape[1]), f32), unroll=4)
    out_ref[...] = (gelu(gate_ref[...].astype(f32)) * b_ref[...]).astype(bf16)


def mixed(gate_rows, input_rows, mix_kernel, w_recur, w_inject, soft):
    length, width = gate_rows.shape
    heads, size, _ = w_recur.shape
    across = pl.BlockSpec((length, size), lambda h: (0, h))
    block = pl.BlockSpec((1, size, size), lambda h: (h, 0, 0))
    return pl.pallas_call(
        mixer_kernel,
        grid=(heads,),
        out_shape=jax.ShapeDtypeStruct((length, width), bf16),
        in_specs=[
            across,
            across,
            pl.BlockSpec((mix_kernel.shape[0], size), lambda h: (0, h)),
            block,
            block,
            pl.BlockSpec((1, size), lambda h: (0, h)),
        ],
        out_specs=across,
        scratch_shapes=[pltpu.VMEM((length, size), f32), pltpu.VMEM((length, size), f32)],
        cost_estimate=pl.CostEstimate(
            flops=20_000_000 * heads, bytes_accessed=4 * length * width * 2, transcendentals=0
        ),
    )(gate_rows, input_rows, mix_kernel, w_recur, w_inject, soft)


def causal_conv(values, kernel):
    length = values.shape[0]
    widths = kernel.shape[0]
    padded = jnp.pad(values.astype(f32), ((widths - 1, 0), (0, 0)))
    weights = kernel.astype(f32)
    result = padded[0:length] * weights[0]
    for offset in range(1, widths):
        result = result + padded[offset : offset + length] * weights[offset]
    return result


def shards(
    n_fs,
    n_tp,
    tokens,
    pre_mix_gain,
    w_gate_in,
    w_input,
    mix_kernel,
    w_recur,
    w_inject,
    decay_param,
    w_mix_out,
    post_mix_gain,
    pre_ffn_gain,
    w_up_gate,
    w_up_value,
    gate_kernel,
    value_kernel,
    w_down,
    post_ffn_gain,
):
    index = lax.axis_index("tp")
    ring = Ring(n_fs)
    length, width = tokens.shape

    gains = jnp.stack([pre_mix_gain, post_mix_gain, pre_ffn_gain])
    gains = jnp.pad(gains, ((0, 13), (0, 0)))
    packed = lax.optimization_barrier(jnp.concatenate([tokens, gains], axis=0))
    far = n_fs // 2
    ins = ring.advance(ring.start("ring_in", [w_input, w_gate_in]), far - 1)
    outs = ring.start("ring_out", [w_mix_out], after=ring.marks(ins))
    ring.advance(ins)
    ring.advance(outs, far - 1)
    ups = ring.start("ring_up", [w_up_gate, w_up_value], after=ring.marks(outs))
    ring.advance(outs)
    in_found, out_found, up_found = ins["found"], outs["found"], ups["found"]
    rows_all = gathered_columns(packed, n_tp, index)
    tokens_all = rows_all[:length]
    pre_mix_all, post_mix_all, pre_ffn_all = rows_all[length], rows_all[length + 1], rows_all[length + 2]

    normed_in = normed_full(tokens_all, pre_mix_all).astype(bf16)
    input_rows = summed_chunks(ring, normed_in, in_found[0])
    gate_rows = summed_chunks(ring, normed_in, in_found[1])
    soft = jax.nn.softplus(-decay_param)[None, :]
    gate_rows = ring.tie(ups, gate_rows)
    ring.advance(ups)
    hidden = mixed(gate_rows, input_rows, mix_kernel, w_recur, w_inject, soft)
    mixer_chunks = ring.tie(ups, placed_chunks(ring, hidden, out_found[0]))
    left = max(far - 3, 0)
    ring.advance(ups, 1 + left)
    mixer_rows = scattered_rows(mixer_chunks, n_tp, index)

    place = jnp.int32(0)
    rows = length
    for bit in bits_up(n_tp):
        rows //= 2
        place = place + ((index & bit) // bit) * rows
    my_tokens = lax.dynamic_slice_in_dim(tokens_all, place, rows, axis=0)
    my_middle = (my_tokens.astype(f32) + normed_full(mixer_rows, post_mix_all)).astype(bf16)
    my_middle = ring.tie(ups, my_middle)
    ring.advance(ups)
    middle = gathered_rows(my_middle, n_tp, index)
    normed_mid = normed_full(middle, pre_ffn_all).astype(bf16)
    ring.advance(ups, far - ups["step"])
    downs = ring.advance(ring.start("ring_down", [w_down]))

    up_gate = summed_chunks(ring, normed_mid, up_found[0])
    later_mid = ring.tie(downs, normed_mid)
    ring.advance(downs, far - 1)
    down_found = downs["found"]
    up_value = summed_chunks(ring, later_mid, up_found[1])
    activated = (
        jax.nn.gelu(causal_conv(up_gate, gate_kernel), approximate=True)
        * causal_conv(up_value, value_kernel)
    ).astype(bf16)
    activated = lax.optimization_barrier(activated)
    ffn_sum = scattered_columns(placed_chunks(ring, activated, down_found[0]), n_tp, index)
    squares = lax.psum(jnp.sum(ffn_sum * ffn_sum, axis=1), "tp")
    factor = lax.rsqrt(squares / (width * n_tp) + norm_eps)
    mine = lax.dynamic_slice_in_dim(middle, index * width, width, axis=1)
    return (
        mine.astype(f32) + ffn_sum * factor[:, None] * post_ffn_gain.astype(f32)[None, :]
    ).astype(bf16)


def solution(mesh):
    def layer(*args):
        return shards(mesh.shape["fs"], mesh.shape["tp"], *args)

    return jax.shard_map(
        layer,
        mesh=mesh,
        in_specs=(
            P("fs", "tp"),
            P("tp"),
            P("fs", "tp"),
            P("fs", "tp"),
            P(None, "tp"),
            P("tp", None, None),
            P("tp", None, None),
            P("tp"),
            P("tp", "fs"),
            P("tp"),
            P("tp"),
            P("fs", "tp"),
            P("fs", "tp"),
            P(None, "tp"),
            P(None, "tp"),
            P("tp", "fs"),
            P("tp"),
        ),
        out_specs=P("fs", "tp"),
        check_vma=False,
    )
```
